32 devices in a mesh: ep: 8 (over z, y), tp: 4 (over x, core).
Axes of the slice: x: 2, y: 2, z: 4, core: 2. Of those that a mesh axis runs over, the one named last changes fastest.
Arguments:
- tokens: bfloat16 [192, 1024], P('ep'), may hold values from -3 to 3
- attn_gain: float32 [1024], replicated, may hold values from 0.1 to 1.9
- w_query: bfloat16 [1024, 1024], P(None, 'tp'), may hold values from -0.1875 to 0.1875
- w_key: bfloat16 [1024, 256], P(None, 'tp'), may hold values from -0.1875 to 0.1875
- w_value: bfloat16 [1024, 256], P(None, 'tp'), may hold values from -0.1875 to 0.1875
- attn_bias: float32 [16], P('tp'), may hold values from -7.5 to -3
- key_cache: bfloat16 [192, 256, 1024], P('ep', 'tp'), may hold values from -6 to 6
- value_cache: bfloat16 [192, 256, 1024], P('ep', 'tp'), may hold values from -6 to 6
- lengths: int32 [192], P('ep'), may hold values from 128 to 1024
- w_out: bfloat16 [1024, 1024], P('tp'), may hold values from -0.75 to 0.75
- ffn_gain: float32 [1024], replicated, may hold values from 0.1 to 1.9
- routes: int32 [192, 2], P('ep'), may hold values from 0 to 7, all different within a row; in each aligned block of 24 rows (0 to 23, 24 to 47, ...) at most 12 rows name the same one
- route_weight: float32 [192, 2], P('ep'), may hold values from 0.2 to 1
- expert_gate: bfloat16 [8, 1024, 3584], P('ep', None, 'tp'), may hold values from -0.1875 to 0.1875
- expert_up: bfloat16 [8, 1024, 3584], P('ep', None, 'tp'), may hold values from -0.1875 to 0.1875
- expert_down: bfloat16 [8, 3584, 1024], P('ep', 'tp'), may hold values from -0.09375 to 0.09375
Outputs:
- mixed: bfloat16 [192, 1024], P('ep')
- new_keys: bfloat16 [192, 256], P('ep', 'tp')
- new_values: bfloat16 [192, 256], P('ep', 'tp')
The draws below stay inside these ranges and needn't reach their ends.
Inputs may be any that keep to these rules, and one draw needn't show every extreme that they name: `routes`: each row names 2 different experts. Among the rows of one device no expert is named by more than 12 of them, and on some device some expert is named by exactly 12.
All inputs are finite; a program needn't handle non-finite values.
Results may differ from the reference program's by a relative error of at most 0.02.
Values may be sent and summed in bfloat16 or wider, within the bound.
A program may use at most 64 MiB of HBM per device.

```python
import math
import jax
import jax.numpy as jnp
import numpy as np
from jax import lax

D = 1024
HEADS = 16
KV_HEADS = 4
HEAD = 64
FF = 3584
TOP = 2
SEQS = 24
LEN = 1024
EXPERTS = 8
CAP = 12
BATCH = 192
N_EP = 8
N_TP = 4


def set_ends(drawn, stream_key, least, top_value):
    dims = drawn.shape
    index_at = [jax.random.randint(jax.random.fold_in(stream_key, axis), (), 0, dims[axis]) for axis in range(len(dims))]
    drawn = drawn.at[tuple(index_at)].set(least)
    longest = dims.index(max(dims))
    index_at[longest] = (index_at[longest] + 1) % dims[longest]
    return drawn.at[tuple(index_at)].set(top_value)


def level_of(stream_key, dims, cuts, low, high):
    def one(dim, shards_of):
        steps = jax.random.uniform(jax.random.fold_in(jax.random.fold_in(stream_key, 6), dim), (shards_of,), jnp.float32, low / len(cuts), high / len(cuts))
        return jnp.repeat(jnp.exp(steps), dims[dim] // shards_of).reshape((-1,) + (1,) * (len(dims) - dim - 1))

    factor_of = one(*cuts[0])
    for cut in cuts[1:]:
        factor_of = factor_of * one(*cut)
    return factor_of


def routed_block(rng, own, number, rows, number_of, top, limit, lean):
    order = jax.random.permutation(rng, number_of)
    heavy_load, usual = shares(number_of, rows * top, limit, lean, True), shares(number_of, rows * top, limit, lean, False)
    places = jnp.arange(number_of)

    def named(sizes, offset_by):
        used = int((sizes > 0).sum())
        fixed = max(1, used // 4)
        passed = fixed + (places - fixed + offset_by * (used - fixed)) % max(1, number_of - fixed)
        return jnp.zeros((number_of,), jnp.int32).at[order[jnp.where(places < fixed, places, passed)]].set(jnp.asarray(sizes, jnp.int32))

    sizes = jnp.where(number % 4 == 0, named(heavy_load, number // 4), named(usual, number - number // 4 - 1))
    mixed = jax.random.permutation(jax.random.fold_in(own, 3), number_of)
    donor, sink = mixed[0:number_of // 2 * 2:2], mixed[1:number_of // 2 * 2:2]
    margin = jnp.minimum(sizes[donor] - 1, limit - sizes[sink]) // 2
    margin = jnp.where((donor == order[0]) | (sink == order[0]) | (sizes[sink] == 0), 0, jnp.maximum(margin, 0))
    passed = jax.random.randint(jax.random.fold_in(own, 4), (number_of // 2,), 0, 1 << 20) % (margin + 1)
    sizes = sizes.at[donor].add(-passed).at[sink].add(passed)
    labels = jnp.searchsorted(jnp.cumsum(sizes), jnp.arange(rows * top), side="right").astype(jnp.int32)
    grid = labels.reshape(top, rows).T
    grid = grid[jax.random.permutation(jax.random.fold_in(own, 1), rows)]
    offset_by = jax.random.randint(jax.random.fold_in(own, 2), (rows, 1), 0, top)
    return jnp.take_along_axis(grid, (jnp.arange(top)[None, :] + offset_by) % top, axis=1)


def shares(amount, total, bound, skew, full):
    portions = [(1 << 20) // math.isqrt(rank ** skew) + 1 for rank in range(1, amount + 1)]
    largest = bound if full else min(bound, max(-(-total // amount), total * portions[0] // sum(portions)))
    least = 1 if total - largest >= amount - 1 else 0
    given, surplus = [largest] + [least] * (amount - 1), total - largest - least * (amount - 1)
    while surplus > 0:
        movable = [i for i in range(1, amount) if given[i] < largest] or [i for i in range(1, amount) if given[i] < bound]
        whole, remaining = sum([portions[i] for i in movable]), surplus
        for i in movable:
            extra = min(bound - given[i], max(1, remaining * portions[i] // whole), surplus)
            given[i] = given[i] + extra
            surplus = surplus - extra
    return np.array(given)


def normal_values(key, shape, scale, most, shards=(), kind=jnp.bfloat16):
    array = scale * jax.random.normal(key, shape, jnp.float32)
    if shards:
        array = array * level_of(key, shape, shards, -0.22, 0.18)
    return jnp.clip(array, -most, most).astype(kind)


def setup_inputs(seed: int = 0) -> dict:
    keys = jax.random.split(jax.random.key(seed), 17)
    tokens = normal_values(keys[0], (BATCH, D), 0.5, 3.0, ((0, 8),))
    attn_gain = jnp.clip(1.0 + 0.18 * jax.random.normal(keys[1], (D,), jnp.float32), 0.1, 1.9)
    w_query = normal_values(keys[2], (D, HEADS * HEAD), D ** -0.5, 0.1875, ((1, 4),))
    w_key = normal_values(keys[3], (D, KV_HEADS * HEAD), D ** -0.5, 0.1875, ((1, 4),))
    w_value = normal_values(keys[4], (D, KV_HEADS * HEAD), D ** -0.5, 0.1875, ((1, 4),))
    attn_bias = jnp.clip(-7.5 + 4.5 * jax.random.uniform(keys[5], (HEADS,), jnp.float32) ** level_of(keys[5], (HEADS,), ((0, 4),), -0.2, 0.2), -7.5, -3.0)
    key_cache = normal_values(keys[6], (BATCH, KV_HEADS * HEAD, LEN), 1.0, 6.0, ((0, 8), (1, 4)))
    value_cache = normal_values(keys[7], (BATCH, KV_HEADS * HEAD, LEN), 1.0, 6.0, ((0, 8), (1, 4)))
    lengths = set_ends(jax.random.randint(keys[8], (BATCH,), LEN // 8, LEN + 1), jax.random.fold_in(keys[8], 1), LEN // 8, LEN).astype(jnp.int32)
    w_out = normal_values(keys[9], (HEADS * HEAD, D), (HEADS * HEAD // 16) ** -0.5, 0.75, ((0, 4),))
    ffn_gain = jnp.clip(1.0 + 0.18 * jax.random.normal(keys[10], (D,), jnp.float32), 0.1, 1.9)
    routes_keys = jax.random.split(jax.random.fold_in(keys[11], 1), BATCH // SEQS)
    routes_turns = jax.random.permutation(jax.random.fold_in(keys[11], 3), BATCH // SEQS)
    routes = jax.vmap(lambda own, number: routed_block(jax.random.fold_in(keys[11], 2), own, number, SEQS, EXPERTS, TOP, CAP, 1))(routes_keys, routes_turns).reshape((BATCH, TOP))
    route_weight = jnp.clip(0.2 + 0.8 * jax.random.uniform(keys[12], (BATCH, TOP), jnp.float32) ** level_of(keys[12], (BATCH, TOP), ((0, 8),), -0.2, 0.2), 0.2, 1.0)
    expert_gate = normal_values(keys[13], (EXPERTS, D, FF), D ** -0.5, 0.1875, ((0, 8), (2, 4)))
    expert_up = normal_values(keys[14], (EXPERTS, D, FF), D ** -0.5, 0.1875, ((0, 8), (2, 4)))
    expert_down = normal_values(keys[15], (EXPERTS, FF, D), FF ** -0.5, 0.09375, ((0, 8), (1, 4)))
    return {"tokens": tokens, "attn_gain": attn_gain, "w_query": w_query, "w_key": w_key, "w_value": w_value, "attn_bias": attn_bias, "key_cache": key_cache, "value_cache": value_cache, "lengths": lengths, "w_out": w_out, "ffn_gain": ffn_gain, "routes": routes, "route_weight": route_weight, "expert_gate": expert_gate, "expert_up": expert_up, "expert_down": expert_down}


norm_epsilon = 1e-06

def rms_scale(inputs, gains):
    widened = inputs.astype(jnp.float32)
    factor = lax.rsqrt(lax.optimization_barrier(jnp.mean(widened * widened, axis=-1, keepdims=True)) + norm_epsilon)
    return (widened * factor * gains).astype(jnp.bfloat16)

def dispatch_matrix(block_routes, experts, capacity):
    flat_routes = block_routes.reshape(-1).astype(jnp.int32)
    onehot = (flat_routes[:, None] == jnp.arange(experts, dtype=jnp.int32)[None, :]).astype(jnp.int32)
    before = (jnp.cumsum(onehot, axis=0) - onehot).astype(jnp.int32)
    slot_index = lax.optimization_barrier(jnp.sum(before * onehot, axis=1)).astype(jnp.int32)
    target = flat_routes * capacity + slot_index
    return jnp.arange(experts * capacity, dtype=jnp.int32)[:, None] == target[None, :]

def stick_read(queries, key_block, value_block, bias_grid, lengths):
    row_count, kv_count, group_size, head_size = queries.shape
    key_span = key_block.shape[2]
    key_heads = key_block.reshape(row_count, kv_count, head_size, key_span).astype(jnp.float32)
    value_heads = value_block.reshape(row_count, kv_count, head_size, key_span).astype(jnp.float32)
    scores = jnp.einsum('skgd,skdl->skgl', queries.astype(jnp.float32), key_heads) * head_size ** (-0.5)
    scores = scores + bias_grid[None, :, :, None]
    inside = (jnp.arange(key_span, dtype=jnp.int32)[None, :] < lengths[:, None])[:, None, None, :]
    log_fall = jnp.where(inside, jax.nn.log_sigmoid(-scores), 0.0)
    log_after = lax.cumsum(log_fall, axis=3, reverse=True) - log_fall
    weights = jnp.where(inside, jnp.exp(jax.nn.log_sigmoid(scores) + log_after), 0.0).astype(jnp.bfloat16)
    mixed_out = jnp.einsum('skgl,skdl->skgd', weights.astype(jnp.float32), value_heads)
    return mixed_out.astype(jnp.bfloat16).reshape(row_count, -1)

def expert_rows(operands):
    row_block, gate_matrix, up_matrix, down_matrix = operands
    gate_act = jnp.dot(row_block, gate_matrix, preferred_element_type=jnp.float32)
    lifted = jnp.dot(row_block, up_matrix, preferred_element_type=jnp.float32)
    hidden = (jax.nn.silu(gate_act) * lifted).astype(jnp.bfloat16)
    pieces = jnp.einsum('rtf,tfd->rtd', hidden.reshape(hidden.shape[0], N_TP, -1).astype(jnp.float32), down_matrix.reshape(N_TP, -1, down_matrix.shape[1]).astype(jnp.float32))
    rounded = lax.optimization_barrier(pieces.astype(jnp.bfloat16))
    return lax.optimization_barrier(jnp.sum(rounded.astype(jnp.float32), axis=1)).astype(jnp.bfloat16)

def block_plan(block_routes):
    return dispatch_matrix(block_routes, EXPERTS, CAP)

def reference(tokens, attn_gain, w_query, w_key, w_value, attn_bias, key_cache, value_cache, lengths, w_out, ffn_gain, routes, route_weight, expert_gate, expert_up, expert_down):
    normed = rms_scale(tokens, attn_gain)
    queries = jnp.dot(normed, w_query, preferred_element_type=jnp.float32).astype(jnp.bfloat16)
    new_keys = jnp.dot(normed, w_key, preferred_element_type=jnp.float32).astype(jnp.bfloat16)
    new_values = jnp.dot(normed, w_value, preferred_element_type=jnp.float32).astype(jnp.bfloat16)
    group_size = HEADS // KV_HEADS
    grouped = queries.reshape(N_EP, SEQS, KV_HEADS, group_size, HEAD)
    bias_grid = attn_bias.reshape(KV_HEADS, group_size)

    def per_block(block_args):
        return stick_read(block_args[0], block_args[1], block_args[2], bias_grid, block_args[3])
    attended = lax.map(per_block, (grouped, key_cache.reshape(N_EP, SEQS, KV_HEADS * HEAD, LEN), value_cache.reshape(N_EP, SEQS, KV_HEADS * HEAD, LEN), lengths.reshape(N_EP, SEQS)))
    attended = attended.reshape(BATCH, HEADS * HEAD)
    parts = jnp.einsum('btf,tfd->btd', attended.reshape(BATCH, N_TP, -1).astype(jnp.float32), w_out.reshape(N_TP, -1, D).astype(jnp.float32))
    rounded = lax.optimization_barrier(parts.astype(jnp.bfloat16))
    attn_total = lax.optimization_barrier(jnp.sum(rounded.astype(jnp.float32), axis=1))
    residual = (tokens.astype(jnp.float32) + attn_total).astype(jnp.bfloat16)
    normed_two = rms_scale(residual, ffn_gain)
    plans = jax.vmap(block_plan)(routes.reshape(N_EP, SEQS, TOP)).astype(jnp.float32)
    repeated = jnp.repeat(normed_two.reshape(N_EP, SEQS, 1, D), TOP, axis=2).reshape(N_EP, SEQS * TOP, D)
    sent = jnp.einsum('per,prd->ped', plans, repeated.astype(jnp.float32)).astype(jnp.bfloat16)
    received = sent.reshape(N_EP, EXPERTS, CAP, D).transpose(1, 0, 2, 3).reshape(EXPERTS, N_EP * CAP, D)
    outputs = lax.map(expert_rows, (received, expert_gate, expert_up, expert_down))
    back = outputs.reshape(EXPERTS, N_EP, CAP, D).transpose(1, 0, 2, 3).reshape(N_EP, EXPERTS * CAP, D)
    picked = jnp.einsum('per,ped->prd', plans, back.astype(jnp.float32)).reshape(BATCH, TOP, D)
    moe_sum = lax.optimization_barrier(jnp.sum(picked * route_weight[:, :, None], axis=1))
    mixed = (residual.astype(jnp.float32) + moe_sum).astype(jnp.bfloat16)
    return (mixed, new_keys, new_values)
```

```python
import functools

import jax
import jax.numpy as jnp
from jax import lax
from jax.experimental import pallas as pl
from jax.experimental.pallas import tpu as pltpu
from jax.sharding import PartitionSpec as P

EPS = 1e-06
F32 = jnp.float32
BF16 = jnp.bfloat16
MESH = pl.DeviceIdType.MESH


def iota(shape, dim):
    return lax.broadcasted_iota(jnp.int32, shape, dim)


def onehot(mask):
    return jnp.where(mask, 1.0, 0.0).astype(BF16)


def dot(a, b):
    return jnp.dot(a, b, preferred_element_type=F32)


def dot_nt(a, b):
    return lax.dot_general(a, b, (((1,), (1,)), ((), ())), preferred_element_type=F32)


def kernel(
    n_ep, n_tp, capacity, cap_pad,
    tokens_hbm, attn_gain_hbm, w_query, w_key, w_value, attn_bias_hbm, key_cache, value_cache, lengths_hbm,
    w_out, ffn_gain_hbm, routes_hbm, route_weight_hbm, gate, up, down,
    mixed, new_keys, new_values,
    tokens, attn_gain, attn_bias, lengths, ffn_gain, routes, route_weight,
    wq, wk, wv, kbuf, vbuf, wo, wg, wu, wd,
    part, parts, outgoing, arrived, passed, share_out, share_in, ret, back, fin_out, finals,
    load_sem, k_sem, v_sem,
    a_send, a_recv, b_send, b_recv, f_send, f_recv, c_send, c_recv, d_send, d_recv, e_send, e_recv,
):
    ep = lax.axis_index("ep")
    tp = lax.axis_index("tp")
    seqs, width = tokens.shape
    head = w_key.shape[0]
    heads = w_query.shape[1] // head
    span = key_cache.shape[2]
    rows = seqs * heads
    depth = seqs * head
    half = width // 2
    total = n_ep * cap_pad
    core = lax.rem(tp, 2)
    mate = tp + 1 - 2 * core
    lanes = 128
    per = lanes // head
    chunks = depth // lanes

    pow2 = n_ep & (n_ep - 1) == 0

    def dest(k):
        if not pow2:
            return lax.rem(ep + k, n_ep)
        other, bit = ep, 1
        while bit < n_ep:
            if k & bit:
                other = other + bit * (1 - 2 * lax.rem(ep // bit, 2))
            bit *= 2
        return other

    def source(k):
        return dest(k) if pow2 else lax.rem(ep + n_ep - k, n_ep)

    loads = {}
    for i, (name, src, dst) in enumerate(
        (("tokens", tokens_hbm, tokens), ("gain", attn_gain_hbm, attn_gain), ("wq", w_query, wq),
         ("bias", attn_bias_hbm, attn_bias), ("lengths", lengths_hbm, lengths), ("fgain", ffn_gain_hbm, ffn_gain),
         ("routes", routes_hbm, routes), ("weights", route_weight_hbm, route_weight),
         ("wk", w_key, wk), ("wv", w_value, wv), ("wo", w_out, wo),
         ("wg", gate.at[0], wg), ("wu", up.at[0], wu), ("wd", down.at[0], wd))
    ):
        loads[name] = pltpu.make_async_copy(src, dst, load_sem.at[i])
    k_parts, v_parts = k_sem.shape[0], k_sem.shape[1]
    k_cols = span // k_parts
    k_rows = seqs // v_parts
    k_loads, v_loads = [], []
    for a in range(k_parts):
        at = pl.ds((k_parts - 1 - a) * k_cols, k_cols)
        k_loads.append([])
        for b in range(v_parts):
            piece = pl.ds(b * k_rows, k_rows)
            k_loads[-1].append(
                pltpu.make_async_copy(key_cache.at[piece, :, at], kbuf.at[piece, :, at], k_sem.at[a, b]))
    for b in range(v_sem.shape[0]):
        piece = pl.ds(b * (seqs // v_sem.shape[0]), seqs // v_sem.shape[0])
        v_loads.append(pltpu.make_async_copy(value_cache.at[piece], vbuf.at[piece], v_sem.at[b]))
    for name in ("tokens", "gain", "wq"):
        loads[name].start()
    for c in k_loads[0]:
        c.start()
    for name in ("bias", "lengths"):
        loads[name].start()
    for group in k_loads[1:]:
        for c in group:
            c.start()

    barrier = pltpu.get_barrier_semaphore()
    for d in range(1, n_tp):
        pl.semaphore_signal(barrier, inc=1, device_id=(ep, lax.rem(tp + d, n_tp)), device_id_type=MESH)
    for k in range(1, n_ep):
        pl.semaphore_signal(barrier, inc=1, device_id=(dest(k), tp), device_id_type=MESH)

    loads["tokens"].wait()
    loads["gain"].wait()
    token_rows = tokens[...].astype(F32)
    factor = lax.rsqrt(jnp.mean(token_rows * token_rows, axis=-1, keepdims=True) + EPS)
    normed = (token_rows * factor * attn_gain[...]).astype(BF16)

    loads["wq"].wait()
    for c in v_loads:
        c.start()
    queries = dot(normed, wq[...]) * (head ** -0.5)
    block_of = iota((seqs, lanes), 1) // head
    seq_of = iota((seqs, lanes), 0)
    spread = []
    for h in range(heads):
        pair = queries[:, (h // per) * lanes:(h // per + 1) * lanes]
        mine = jnp.zeros_like(pair)
        for j in range(per):
            shift = ((j - h % per) * head) % lanes
            turned = pltpu.roll(pair, shift, 1) if shift else pair
            mine = jnp.where(block_of == j, turned, mine)
        spread.append(mine)
    masks = [seq_of == block_of + c * per for c in range(chunks)]
    diag = jnp.concatenate(
        [jnp.concatenate([jnp.where(m, q, 0.0) for m in masks], axis=1) for q in spread], axis=0).astype(BF16)

    loads["bias"].wait()
    loads["lengths"].wait()
    bias_col = jnp.concatenate(
        [jnp.broadcast_to(attn_bias[0:1, h:h + 1], (seqs, 1)) for h in range(heads)], axis=0)
    same = iota((seqs, seqs), 0) == iota((seqs, seqs), 1)
    len_one = jnp.sum(jnp.where(same, lengths[...].astype(F32), 0.0), axis=1, keepdims=True)
    len_col = jnp.concatenate([len_one] * heads, axis=0)
    block_len = 256 if k_cols % 256 == 0 else k_cols
    later = onehot(iota((block_len, block_len), 0) > iota((block_len, block_len), 1))
    position = iota((rows, block_len), 1).astype(F32)
    weights = []
    offset = jnp.zeros((rows, 1), F32)
    for a in range(k_parts):
        for c in k_loads[a]:
            c.wait()
        first_col = (k_parts - 1 - a) * k_cols
        scores = dot(diag, kbuf[:, :, first_col:first_col + k_cols].reshape(depth, k_cols)) + bias_col
        for j in reversed(range(k_cols // block_len)):
            s = scores[:, j * block_len:(j + 1) * block_len]
            inside = position < len_col - float(first_col + j * block_len)
            soft = jnp.log(1.0 + jnp.exp(-jnp.abs(s)))
            fall = jnp.where(inside, -(jnp.maximum(s, 0.0) + soft), 0.0)
            rise = jnp.minimum(s, 0.0) - soft
            high = fall.astype(BF16)
            low = (fall - high.astype(F32)).astype(BF16)
            both = dot(jnp.concatenate([high, low], axis=0), later)
            after = both[:rows] + both[rows:]
            w = jnp.exp(rise + (after + offset))
            weights.insert(0, jnp.where(inside, w, 0.0).astype(BF16))
            offset = offset + after[:, 0:1] + fall[:, 0:1]
    weights = jnp.concatenate(weights, axis=1)

    loads["wo"].start()
    for name in ("wk", "wv", "fgain", "routes", "weights", "wg", "wu", "wd"):
        loads[name].start()
    folded = [jnp.zeros((seqs, lanes), F32) for _ in range(heads)]
    per_group = max(1, 256 // head)
    for c in v_loads:
        c.wait()
    for g in range(seqs // per_group):
        found = dot_nt(weights, vbuf[g * per_group:(g + 1) * per_group].reshape(per_group * head, span))
        for c in range(per_group // per):
            m = masks[g * (per_group // per) + c]
            for h in range(heads):
                folded[h] = folded[h] + jnp.where(
                    m, found[h * seqs:(h + 1) * seqs, c * lanes:(c + 1) * lanes], 0.0)
    attended = []
    for p in range(heads // per):
        mine = jnp.zeros((seqs, lanes), F32)
        for j in range(per):
            one = folded[p * per + j]
            full = one
            for t in range(1, per):
                full = full + pltpu.roll(one, t * head, 1)
            mine = jnp.where(block_of == j, full, mine)
        attended.append(mine)
    attended = jnp.concatenate(attended, axis=1).astype(BF16)
    loads["wo"].wait()
    made = dot(attended, wo[...]).astype(BF16)
    part[0] = made[:, :half]
    part[1] = made[:, half:]

    pl.semaphore_wait(barrier, n_tp - 1 + n_ep - 1)
    sends = []
    tp_order = list(range(2, n_tp)) + [1] if n_tp > 2 else [1]

    def tp_peer(d):
        chip = lax.rem(tp // 2 + d // 2, n_tp // 2)
        return 2 * chip + lax.rem(core + d, 2)

    def tp_source(d):
        chip = lax.rem(tp // 2 + n_tp // 2 - d // 2, n_tp // 2)
        return 2 * chip + lax.rem(core + d, 2)

    for d in tp_order:
        peer = tp_peer(d)
        c = pltpu.make_async_remote_copy(
            part.at[lax.rem(core + d, 2)], parts.at[d], a_send.at[d], a_recv.at[d],
            device_id=(ep, peer), device_id_type=MESH)
        c.start()
        sends.append(c)

    loads["routes"].wait()
    loads["weights"].wait()
    loads["wk"].wait()
    loads["wv"].wait()
    slot_rows = iota((total, seqs), 0)
    if pow2:
        expert = jnp.bitwise_xor(slot_rows // cap_pad, ep)
    else:
        expert = lax.rem(slot_rows // cap_pad + ep, n_ep)
    first = routes[0:1, :] == expert
    named = first | (routes[1:2, :] == expert)
    earlier = onehot(iota((seqs, seqs), 0) < iota((seqs, seqs), 1))
    before = dot(onehot(named), earlier)
    planned = jnp.where(named & (before == (slot_rows % cap_pad).astype(F32)), 1.0, 0.0)
    plan = planned.astype(BF16)
    mixing = (planned * jnp.where(first, route_weight[0:1, :], route_weight[1:2, :])).T
    mix_high = mixing.astype(BF16)
    mix_low = (mixing - mix_high.astype(F32)).astype(BF16)
    mix = jnp.concatenate([mix_high.astype(F32), mix_low.astype(F32)], axis=0).astype(BF16)
    new_keys[...] = dot_nt(normed, wk[...]).astype(BF16)
    new_values[...] = dot_nt(normed, wv[...]).astype(BF16)
    at_own = pl.ds(pl.multiple_of(core * half, half), half)
    at_mate = pl.ds(pl.multiple_of((1 - core) * half, half), half)
    attn_total = tokens[:, at_own].astype(F32) + part[core].astype(F32)

    for d in tp_order[::-1]:
        pltpu.make_async_remote_copy(
            part.at[core], parts.at[d], a_send.at[d], a_recv.at[d],
            device_id=(ep, tp_source(d)), device_id_type=MESH).wait_recv()
        attn_total = attn_total + parts[d].astype(F32)
    residual = attn_total.astype(BF16)
    outgoing[...] = dot(plan, residual).astype(BF16).reshape(n_ep, cap_pad, half)

    def cut(ref, k):
        return ref.at[k]

    for k in reversed(range(1, n_ep)):
        c = pltpu.make_async_remote_copy(
            cut(outgoing, k), cut(arrived, k), b_send.at[k], b_recv.at[k],
            device_id=(dest(k), tp), device_id_type=MESH)
        c.start()
        sends.append(c)
    c = pltpu.make_async_remote_copy(
        cut(outgoing, 0), cut(passed, 0), f_send.at[0], f_recv.at[0], device_id=(ep, mate), device_id_type=MESH)
    c.start()
    sends.append(c)
    swaps = [c]
    arrived[0] = outgoing[0]
    loads["fgain"].wait()
    loads["wg"].wait()
    loads["wu"].wait()
    loads["wd"].wait()
    for k in range(1, n_ep):
        pltpu.make_async_remote_copy(
            cut(outgoing, k), cut(arrived, k), b_send.at[k], b_recv.at[k],
            device_id=(source(k), tp), device_id_type=MESH).wait_recv()
        c = pltpu.make_async_remote_copy(
            cut(arrived, k), cut(passed, k), f_send.at[k], f_recv.at[k],
            device_id=(ep, mate), device_id_type=MESH)
        c.start()
        sends.append(c)
        swaps.append(c)
    x = arrived[...].reshape(total, half).astype(F32)
    square = jnp.sum(x * x, axis=-1, keepdims=True)
    x = (x * ffn_gain[:, at_own]).astype(BF16)
    gated = dot(x, wg[at_own, :])
    lifted = dot(x, wu[at_own, :])
    for c in swaps:
        c.wait_recv()
    x = passed[...].reshape(total, half).astype(F32)
    square = square + jnp.sum(x * x, axis=-1, keepdims=True)
    x = (x * ffn_gain[:, at_mate]).astype(BF16)
    factor = lax.rsqrt(square * (1.0 / width) + EPS)
    gated = (gated + dot(x, wg[at_mate, :])) * factor
    lifted = (lifted + dot(x, wu[at_mate, :])) * factor
    hidden = (gated / (1.0 + jnp.exp(-gated)) * lifted).astype(BF16)
    share_out[...] = dot(hidden, wd[:, at_mate]).astype(BF16).reshape(n_ep, cap_pad, half)
    far = n_ep // 2
    pieces = [pl.ds(far, n_ep - far), pl.ds(0, far)]
    pair = []
    for i, piece in enumerate(pieces):
        c = pltpu.make_async_remote_copy(
            share_out.at[piece], share_in.at[piece], c_send.at[i], c_recv.at[i],
            device_id=(ep, mate), device_id_type=MESH)
        c.start()
        sends.append(c)
        pair.append(c)
    own = dot(hidden, wd[:, at_own]).reshape(n_ep, cap_pad, half)
    for i, (lo, hi) in enumerate(((far, n_ep), (0, far))):
        pair[i].wait_recv()
        ret[lo:hi] = (own[lo:hi] + share_in[lo:hi].astype(F32)).astype(BF16)
        for k in reversed(range(max(lo, 1), hi)):
            c = pltpu.make_async_remote_copy(
                cut(ret, k), cut(back, k), d_send.at[k], d_recv.at[k],
                device_id=(source(k), tp), device_id_type=MESH)
            c.start()
            sends.append(c)
    back[0] = ret[0]
    for k in range(1, n_ep):
        pltpu.make_async_remote_copy(
            cut(ret, k), cut(back, k), d_send.at[k], d_recv.at[k],
            device_id=(dest(k), tp), device_id_type=MESH).wait_recv()
    flat = back[...].reshape(total, half)
    both = dot(mix, flat)
    chips = n_tp // 2
    share = (residual.astype(F32) * (1.0 / chips) + (both[:seqs] + both[seqs:])).astype(BF16)
    fin_out[...] = share
    finals[tp] = share
    for d in tp_order:
        c = pltpu.make_async_remote_copy(
            fin_out, finals.at[tp], e_send.at[d], e_recv.at[d],
            device_id=(ep, tp_peer(d)), device_id_type=MESH)
        c.start()
        sends.append(c)
    for d in tp_order[::-1]:
        src = tp_source(d)
        pltpu.make_async_remote_copy(
            fin_out, finals.at[src], e_send.at[d], e_recv.at[d],
            device_id=(ep, src), device_id_type=MESH).wait_recv()
    for c in range(2):
        value = finals[c].astype(F32)
        for x in range(1, chips):
            value = value + finals[2 * x + c].astype(F32)
        mixed[:, c * half:(c + 1) * half] = value.astype(BF16)
    for c in sends:
        c.wait_send()


def finish(mixed_in, keys_in, values_in, mixed, keys, values, sem):
    copies = [
        pltpu.make_async_copy(a, b, sem.at[i])
        for i, (a, b) in enumerate(((mixed_in, mixed), (keys_in, keys), (values_in, values)))
    ]
    for c in copies:
        c.start()
    for c in copies:
        c.wait()


def solution(mesh):
    n_ep, n_tp = mesh.shape["ep"], mesh.shape["tp"]

    def body(tokens, attn_gain, w_query, w_key, w_value, attn_bias, key_cache, value_cache, lengths,
             w_out, ffn_gain, routes, route_weight, gate, up, down):
        seqs, width = tokens.shape
        top = routes.shape[1]
        capacity = max(2, 2 * seqs * top // n_ep)
        cap_pad = -(-capacity // 16) * 16
        half = width // 2
        head = w_key.shape[1]
        units = gate.shape[2]
        vmem = pl.BlockSpec(memory_space=pltpu.VMEM)
        hbm = pl.BlockSpec(memory_space=pl.ANY)
        sem = pltpu.SemaphoreType.DMA
        args = (tokens, attn_gain[None, :], w_query, w_key.T, w_value.T, attn_bias[None, :], key_cache, value_cache,
                lengths[None, :], w_out, ffn_gain[None, :], routes.T, route_weight.T, gate, up, down)
        exchange = pltpu.VMEM((n_ep, cap_pad, half), BF16)
        outs = pl.pallas_call(
            functools.partial(kernel, n_ep, n_tp, capacity, cap_pad),
            out_shape=(
                pltpu.VMEM((seqs, width), BF16),
                pltpu.VMEM((seqs, head), BF16),
                pltpu.VMEM((seqs, head), BF16),
            ),
            in_specs=[hbm] * len(args),
            out_specs=(vmem, vmem, vmem),
            scratch_shapes=[
                pltpu.VMEM(tokens.shape, BF16),
                pltpu.VMEM((1, width), F32),
                pltpu.VMEM((1, attn_bias.shape[0]), F32),
                pltpu.VMEM((1, seqs), jnp.int32),
                pltpu.VMEM((1, width), F32),
                pltpu.VMEM((top, seqs), jnp.int32),
                pltpu.VMEM((top, seqs), F32),
                pltpu.VMEM(w_query.shape, BF16),
                pltpu.VMEM((head, width), BF16),
                pltpu.VMEM((head, width), BF16),
                pltpu.VMEM(key_cache.shape, BF16),
                pltpu.VMEM(value_cache.shape, BF16),
                pltpu.VMEM(w_out.shape, BF16),
                pltpu.VMEM((width, units), BF16),
                pltpu.VMEM((width, units), BF16),
                pltpu.VMEM((units, width), BF16),
                pltpu.VMEM((2, seqs, half), BF16),
                pltpu.VMEM((n_tp, seqs, half), BF16),
                exchange, exchange, exchange, exchange, exchange, exchange, exchange,
                pltpu.VMEM((seqs, half), BF16),
                pltpu.VMEM((n_tp, seqs, half), BF16),
                sem((14,)), sem((2, 3)), sem((3,)),
                sem((n_tp,)), sem((n_tp,)), sem((n_ep,)), sem((n_ep,)), sem((n_ep,)), sem((n_ep,)),
                sem((2,)), sem((2,)), sem((n_ep,)), sem((n_ep,)), sem((n_tp,)), sem((n_tp,)),
            ],
            compiler_params=pltpu.CompilerParams(
                collective_id=0, has_side_effects=True, vmem_limit_bytes=60 * 1024 * 1024),
        )(*args)
        return pl.pallas_call(
            finish,
            out_shape=tuple(jax.ShapeDtypeStruct(x.shape, x.dtype) for x in outs),
            in_specs=[vmem] * 3,
            out_specs=(hbm,) * 3,
            scratch_shapes=[sem((3,))],
        )(*[pltpu.with_memory_space_constraint(x, pltpu.VMEM) for x in outs])

    return jax.shard_map(
        body,
        mesh=mesh,
        in_specs=(
            P("ep", None), P(), P(None, "tp"), P(None, "tp"), P(None, "tp"), P("tp"),
            P("ep", "tp", None), P("ep", "tp", None), P("ep"), P("tp", None), P(),
            P("ep", None), P("ep", None),
            P("ep", None, "tp"), P("ep", None, "tp"), P("ep", "tp", None),
        ),
        out_specs=(P("ep", None), P("ep", "tp"), P("ep", "tp")),
        check_vma=False,
    )
```
